32 devices in a mesh: grp: 2 (over x), tp: 16 (over z, y, core).
Axes of the slice: x: 2, y: 2, z: 4, core: 2. Of those that a mesh axis runs over, the one named last changes fastest.
Arguments:
- tokens: bfloat16 [160, 2048], P('grp', 'tp'), parts along dimension 0, may hold values from -6 to 6
- lengths: int32 [160], P('grp'), parts along dimension 0, may hold values from 1 to 4096, 81920 in all
- cell_memory: float32 [2, 160, 2048, 256], P(None, 'grp', 'tp'), parts along dimension 1, may hold values from -0.6 to 0.6
- key_sums: float32 [2, 160, 2048], P(None, 'grp', 'tp'), parts along dimension 1, may hold values from -3 to 3
- stabilizer: float32 [2, 160, 8], P(None, 'grp'), parts along dimension 1, may hold values from -3 to 1
- norm_gain: bfloat16 [2, 2048], replicated, may hold values from 0.099609375 to 1.8984375
- query_weight: bfloat16 [2, 2048, 2048], P(None, None, 'tp'), may hold values from -0.125 to 0.125
- key_weight: bfloat16 [2, 2048, 2048], P(None, None, 'tp'), may hold values from -0.125 to 0.125
- value_weight: bfloat16 [2, 2048, 2048], P(None, None, 'tp'), may hold values from -0.125 to 0.125
- outgate_weight: bfloat16 [2, 2048, 2048], P(None, None, 'tp'), may hold values from -0.125 to 0.125
- ingate_weight: bfloat16 [2, 2048, 8], replicated, may hold values from -0.125 to 0.125
- forget_weight: bfloat16 [2, 2048, 8], replicated, may hold values from -0.125 to 0.125
- ingate_bias: float32 [2, 8], replicated, may hold values from -3 to 3
- forget_bias: float32 [2, 8], replicated, may hold values from -1 to 4
- forget_slope: float32 [2, 8], replicated, may hold values from -3 to 3
- head_gain: bfloat16 [2, 2048], P(None, 'tp'), may hold values from 0.099609375 to 1.8984375
- output_weight: bfloat16 [2, 2048, 2048], P(None, None, 'tp'), may hold values from -0.125 to 0.125
Outputs:
- new_tokens: bfloat16 [160, 2048], P('grp', 'tp'), parts along dimension 0
- new_memory: float32 [2, 160, 2048, 256], P(None, 'grp', 'tp'), parts along dimension 1
- new_key_sums: float32 [2, 160, 2048], P(None, 'grp', 'tp'), parts along dimension 1
- new_stabilizer: float32 [2, 160, 8], P(None, 'grp'), parts along dimension 1
The draws below stay inside these ranges and needn't reach their ends.
There are 2 independent parts, one for each index of `grp`. The reference program is written for one: setup_inputs(seed, part) draws one part's arguments, and reference() takes and returns one part's arrays. A program takes and returns all parts, laid end to end along the dimension named above; an argument that names none is the same for every part. Nothing has to cross between parts.
Inputs may be any that keep to these rules, and one draw needn't show every extreme that they name: Each part's 80 lengths sum to 81920, and the largest is exactly 4096.
All inputs are finite; a program needn't handle non-finite values.
Results may differ from the reference program's by a relative error of at most 0.018.
Values may be sent and summed in bfloat16 or wider, within the bound.
A program may use at most 128 MiB of HBM per device.

```python
import math
import jax
import jax.numpy as jnp
import numpy as np
from jax import lax

HEADS = 8
HEAD = 256
D = 2048
BATCH = 80
BLOCKS = 2
MEANLEN = 1024
MAXLEN = 4096


def shard_levels(stream_key, dims, shards, low, high):
    gain, own = 1.0, jax.random.fold_in(stream_key, 6)
    for dim, parts in shards:
        heights = jnp.exp(jax.random.uniform(jax.random.fold_in(own, dim), (parts,), jnp.float32, low / len(shards), high / len(shards)))
        gain = gain * jnp.repeat(heights, dims[dim] // parts).reshape([-1 if axis == dim else 1 for axis in range(len(dims))])
    return gain


def split_up(count, total, most, skew):
    portions = [(1 << 20) // math.isqrt(standing ** skew) + 1 for standing in range(2, count + 1)]
    rest, given = total - most - (count - 1), [1] * (count - 1)
    while rest > 0:
        movable = [i for i in range(count - 1) if given[i] < most]
        pool, budget = sum([portions[i] for i in movable]), rest
        for i in movable:
            addition = min(most - given[i], max(1, budget * portions[i] // pool), rest)
            given[i] = given[i] + addition
            rest = rest - addition
    return np.array([most] + given)


def uneven_parts(own_key, amount, total, reach, slope):
    if amount == 2:
        one = jax.random.randint(own_key, (), max(1, total - reach), min(reach, total - 1) + 1)
        return jnp.stack([one, total - one])
    sizes = jnp.asarray(split_up(amount, total, reach, slope), jnp.int32)
    pairs = (amount - 1) // 2
    donor, taker = sizes[1:1 + 2 * pairs:2], sizes[2:2 + 2 * pairs:2]
    margin = jnp.minimum(donor - 1, reach - taker)
    moved = jax.random.randint(jax.random.fold_in(own_key, 1), (pairs,), 0, 1 << 20) % (margin + 1)
    sizes = sizes.at[1:1 + 2 * pairs:2].set(donor - moved).at[2:2 + 2 * pairs:2].set(taker + moved)
    return sizes[jax.random.permutation(jax.random.fold_in(own_key, 2), amount)]


def scatter_about(stream_key, dims, width, reach, cuts=(), held_as=jnp.bfloat16):
    result = width * jax.random.normal(stream_key, dims, jnp.float32)
    if cuts:
        result = result * shard_levels(stream_key, dims, cuts, -0.22, 0.18)
    return jnp.clip(result, -reach, reach).astype(held_as)


def setup_inputs(seed: int = 0, part: int = 0) -> dict:
    streams_of = jax.random.split(jax.random.key(seed), 18)
    own_keys = jax.random.split(jax.random.fold_in(streams_of[17], part), 18)
    tokens = scatter_about(own_keys[0], (BATCH, D), 1.0, 6.0, ((1, 16),))
    lengths = uneven_parts(own_keys[1], BATCH, BATCH * MEANLEN, MAXLEN, 2).astype(jnp.int32)
    cell_memory = scatter_about(own_keys[2], (BLOCKS, BATCH, D, HEAD), 0.1, 0.6, ((2, 16),), jnp.float32)
    key_sums = scatter_about(own_keys[3], (BLOCKS, BATCH, D), 0.5, 3.0, ((2, 16),), jnp.float32)
    stabilizer = jnp.clip(jax.random.uniform(own_keys[4], (BLOCKS, BATCH, HEADS), jnp.float32, -3.0, 1.0), -3.0, 1.0)
    norm_gain = jnp.clip(1.0 + 0.18 * jax.random.normal(streams_of[5], (BLOCKS, D), jnp.float32), 0.099609375, 1.8984375).astype(jnp.bfloat16)
    query_weight = scatter_about(streams_of[6], (BLOCKS, D, D), D ** -0.5, 0.125, ((2, 16),))
    key_weight = scatter_about(streams_of[7], (BLOCKS, D, D), D ** -0.5, 0.125, ((2, 16),))
    value_weight = scatter_about(streams_of[8], (BLOCKS, D, D), D ** -0.5, 0.125, ((2, 16),))
    outgate_weight = scatter_about(streams_of[9], (BLOCKS, D, D), D ** -0.5, 0.125, ((2, 16),))
    ingate_weight = scatter_about(streams_of[10], (BLOCKS, D, HEADS), D ** -0.5, 0.125)
    forget_weight = scatter_about(streams_of[11], (BLOCKS, D, HEADS), D ** -0.5, 0.125)
    ingate_bias = scatter_about(streams_of[12], (BLOCKS, HEADS), 1.0, 3.0, (), jnp.float32)
    forget_bias = jnp.clip(jax.random.uniform(streams_of[13], (BLOCKS, HEADS), jnp.float32, -1.0, 4.0), -1.0, 4.0)
    forget_slope = jnp.clip(jax.random.uniform(streams_of[14], (BLOCKS, HEADS), jnp.float32, -3.0, 3.0), -3.0, 3.0)
    head_gain = jnp.clip(1.0 + 0.18 * jax.random.normal(streams_of[15], (BLOCKS, D), jnp.float32), 0.099609375, 1.8984375).astype(jnp.bfloat16)
    output_weight = scatter_about(streams_of[16], (BLOCKS, D, D), D ** -0.5, 0.125, ((2, 16),))
    return dict(tokens=tokens, lengths=lengths, cell_memory=cell_memory, key_sums=key_sums, stabilizer=stabilizer, norm_gain=norm_gain, query_weight=query_weight, key_weight=key_weight, value_weight=value_weight, outgate_weight=outgate_weight, ingate_weight=ingate_weight, forget_weight=forget_weight, ingate_bias=ingate_bias, forget_bias=forget_bias, forget_slope=forget_slope, head_gain=head_gain, output_weight=output_weight)


EPS = 1e-05

def one_block(tokens, position, memory, key_sums, stabilizer, norm_gain, query_weight, key_weight, value_weight, outgate_weight, ingate_weight, forget_weight, ingate_bias, forget_bias, forget_slope, head_gain, output_weight):
    batch_rows = tokens.shape[0]
    model_width = tokens.shape[1]
    head_count = stabilizer.shape[1]
    head_size = model_width // head_count
    tok_float = tokens.astype(jnp.float32)
    normed = (tok_float * lax.rsqrt(lax.optimization_barrier(jnp.mean(tok_float * tok_float, axis=-1, keepdims=True)) + EPS) * norm_gain.astype(jnp.float32)).astype(jnp.bfloat16)
    queries = jnp.dot(normed, query_weight, preferred_element_type=jnp.float32).astype(jnp.bfloat16)
    key_rows = (jnp.dot(normed, key_weight, preferred_element_type=jnp.float32) * head_size ** (-0.5)).astype(jnp.bfloat16)
    values = jnp.dot(normed, value_weight, preferred_element_type=jnp.float32).astype(jnp.bfloat16)
    outgate = jnp.dot(normed, outgate_weight, preferred_element_type=jnp.float32).astype(jnp.bfloat16)
    ingate = jnp.dot(normed, ingate_weight, preferred_element_type=jnp.float32) + ingate_bias
    forget = jax.nn.log_sigmoid(jnp.dot(normed, forget_weight, preferred_element_type=jnp.float32) + forget_bias + forget_slope * position[:, None])
    stab_new = jnp.maximum(forget + stabilizer, ingate)
    decays = jnp.exp(forget + stabilizer - stab_new)
    in_weight = jnp.exp(ingate - stab_new)
    query_heads = queries.astype(jnp.float32).reshape(batch_rows, head_count, head_size)
    key_heads = key_rows.astype(jnp.float32).reshape(batch_rows, head_count, head_size)
    value_heads = values.astype(jnp.float32).reshape(batch_rows, head_count, head_size)
    old_memory = memory.reshape(batch_rows, head_count, head_size, head_size)
    mem_new = decays[:, :, None, None] * old_memory + in_weight[:, :, None, None] * value_heads[:, :, :, None] * key_heads[:, :, None, :]
    sums_new = decays[:, :, None] * key_sums.reshape(batch_rows, head_count, head_size) + in_weight[:, :, None] * key_heads
    numerator = jnp.einsum('bhvk,bhk->bhv', mem_new, query_heads, precision=lax.Precision.HIGHEST)
    denominator = jnp.maximum(jnp.abs(lax.optimization_barrier(jnp.sum(sums_new * query_heads, axis=-1))), 1.0)
    hidden = numerator / denominator[:, :, None]
    gated_out = (hidden.reshape(batch_rows, model_width) * head_gain.astype(jnp.float32) * jax.nn.sigmoid(outgate.astype(jnp.float32))).astype(jnp.bfloat16)
    new_tokens = (tok_float + jnp.dot(gated_out, output_weight, preferred_element_type=jnp.float32)).astype(jnp.bfloat16)
    return (new_tokens, mem_new.reshape(batch_rows, model_width, head_size), sums_new.reshape(batch_rows, model_width), stab_new)

def reference(tokens, lengths, cell_memory, key_sums, stabilizer, norm_gain, query_weight, key_weight, value_weight, outgate_weight, ingate_weight, forget_weight, ingate_bias, forget_bias, forget_slope, head_gain, output_weight):
    position = lengths.astype(jnp.float32) / MAXLEN
    current = tokens
    memories, sums_list, stabs = ([], [], [])
    for block_id in range(BLOCKS):
        current, mem_new, sums_new, stab_new = one_block(current, position, cell_memory[block_id], key_sums[block_id], stabilizer[block_id], norm_gain[block_id], query_weight[block_id], key_weight[block_id], value_weight[block_id], outgate_weight[block_id], ingate_weight[block_id], forget_weight[block_id], ingate_bias[block_id], forget_bias[block_id], forget_slope[block_id], head_gain[block_id], output_weight[block_id])
        memories.append(mem_new)
        sums_list.append(sums_new)
        stabs.append(stab_new)
    return (current, jnp.stack(memories), jnp.stack(sums_list), jnp.stack(stabs))
```

```python
import functools

import jax
import jax.numpy as jnp
from jax import lax
from jax.experimental import pallas as pl
from jax.experimental.pallas import tpu as pltpu
from jax.sharding import PartitionSpec as P

HEADS = 8
HEAD = 256
MAXLEN = 4096
EPS = 1e-05
MESH = pl.DeviceIdType.MESH
F32 = jnp.float32
BF16 = jnp.bfloat16
GROUP = 8


def kernel(
    n,
    tokens,
    lengths,
    cell_memory,
    key_sums,
    stabilizer,
    norm_gain,
    query_weight,
    key_weight,
    value_weight,
    outgate_weight,
    ingate_weight,
    forget_weight,
    ingate_bias,
    forget_bias,
    forget_slope,
    head_gain,
    output_weight,
    new_tokens,
    mem,
    new_sums,
    new_stab,
    lengths_in,
    stabilizer_in,
    norm_gain_in,
    ingate_bias_in,
    forget_bias_in,
    forget_slope_in,
    head_gain_in,
    wbig,
    wout,
    wgi,
    wgf,
    wgate,
    small_sem,
    gath,
    pair,
    sums,
    vt_ref,
    decay_ref,
    kk_ref,
    local_sem,
    mem_sem,
    gsend,
    gfwd,
    grecv,
    psend,
    precv,
    ssend,
    srecv,
):
    blocks, batch, rows, head = mem.shape
    heads = stabilizer.shape[1]
    width = output_weight.shape[1]
    split = n // heads
    chips = n // 2
    me = lax.axis_index("tp")
    chip = me // 2
    core = lax.rem(me, 2)
    sibling = me + 1 - 2 * core
    own_head = me // split
    lanes = pl.multiple_of

    def target(j):
        return lax.rem(chip + j, chips) * 2 + core

    def source(j):
        return lax.rem(chip + chips - j, chips) * 2 + core

    own_copy = pltpu.make_async_copy(tokens, gath.at[0, me], local_sem.at[0, 7])
    own_copy.start()
    sums_copy = pltpu.make_async_copy(key_sums, sums.at[core], local_sem.at[1, 7])
    sums_copy.start()
    small = [
        pltpu.make_async_copy(a, b, small_sem.at[i])
        for i, (a, b) in enumerate(
            (
                (lengths, lengths_in),
                (stabilizer, stabilizer_in),
                (norm_gain, norm_gain_in),
                (ingate_bias, ingate_bias_in),
                (forget_bias, forget_bias_in),
                (forget_slope, forget_slope_in),
                (head_gain, head_gain_in),
            )
        )
    ]
    for c in small:
        c.start()
    wcopies, mcopies = [], []
    for l in range(blocks):
        now = []
        for i, w in enumerate((query_weight, key_weight, value_weight, outgate_weight)):
            now.append(
                pltpu.make_async_copy(
                    w.at[l], wbig.at[l, :, pl.ds(i * rows, rows)], local_sem.at[l, i]
                )
            )
        now.append(pltpu.make_async_copy(ingate_weight.at[l], wgi.at[l], local_sem.at[l, 4]))
        now.append(pltpu.make_async_copy(forget_weight.at[l], wgf.at[l], local_sem.at[l, 5]))
        now.append(pltpu.make_async_copy(output_weight.at[l], wout.at[l], local_sem.at[l, 6]))
        wcopies.append(now)
        mcopies.append(pltpu.make_async_copy(cell_memory.at[l], mem.at[l], mem_sem.at[l]))
        for c in now:
            c.start()
        mcopies[l].start()

    barrier = pltpu.get_barrier_semaphore()
    pl.semaphore_signal(barrier, inc=1, device_id={"tp": sibling}, device_id_type=MESH)
    for j in range(1, chips):
        pl.semaphore_signal(barrier, inc=1, device_id={"tp": target(j)}, device_id_type=MESH)
    pl.semaphore_wait(barrier, chips)

    def block_copy(g, slot, sems, k, dest):
        return pltpu.make_async_remote_copy(
            src_ref=gath.at[g, slot],
            dst_ref=gath.at[g, slot],
            send_sem=sems.at[g, k],
            recv_sem=grecv.at[g, slot],
            device_id={"tp": dest},
            device_id_type=MESH,
        )

    sent = []

    def send_own(g):
        for j in range(1, chips):
            c = block_copy(g, me, gsend, j, target(j))
            c.start()
            sent.append(c)
        c = block_copy(g, me, gsend, 0, sibling)
        c.start()
        sent.append(c)

    def arrive(g, step):
        total = None
        block_copy(g, sibling, gsend, 0, sibling).wait_recv()
        total = step(chip, total)
        for j in range(1, chips):
            s = source(j)
            block_copy(g, s, gsend, j, sibling).wait_recv()
            c = block_copy(g, s, gfwd, j, sibling)
            c.start()
            sent.append(c)
        for j in range(1, chips):
            s = source(j)
            block_copy(g, s + 1 - 2 * core, gsend, j, sibling).wait_recv()
            total = step(s // 2, total)
        return total

    own_copy.wait()
    send_own(0)
    sums_copy.wait()
    sums_send = pltpu.make_async_remote_copy(
        src_ref=sums.at[core],
        dst_ref=sums.at[core],
        send_sem=ssend,
        recv_sem=srecv,
        device_id={"tp": sibling},
        device_id_type=MESH,
    )
    sums_send.start()

    for c in small:
        c.wait()
    eye = lax.broadcasted_iota(jnp.int32, (batch, batch), 0) == lax.broadcasted_iota(
        jnp.int32, (batch, batch), 1
    )
    position = jnp.sum(
        jnp.where(eye, lengths_in[...].astype(F32) / MAXLEN, 0.0), axis=1, keepdims=True
    )
    head_mask = lax.broadcasted_iota(jnp.int32, (batch, heads), 1) == own_head
    current = gath[0, me].astype(F32)

    for l in range(blocks):
        for c in wcopies[l][:6]:
            c.wait()
        wgate[l] = jnp.concatenate((wgi[l].astype(F32), wgf[l].astype(F32)), axis=0).astype(BF16)
        old_stab = stabilizer_in[l].T

        def project(c, total, l=l):
            at = pl.ds(lanes(c * 2 * rows, 2 * rows), 2 * rows)
            x = jnp.concatenate((gath[2 * l, 2 * c], gath[2 * l, 2 * c + 1]), axis=1).astype(F32)
            gain = norm_gain_in[:, at].astype(F32)[l : l + 1]
            scaled = (x * gain).astype(BF16)
            part = jnp.dot(scaled, wbig[l, at, :], preferred_element_type=F32)
            gpart = lax.dot_general(
                scaled, wgate[l, :, at], (((1,), (1,)), ((), ())), preferred_element_type=F32
            )
            square = x * x
            if total is None:
                return part, gpart, square
            return total[0] + part, total[1] + gpart, total[2] + square

        proj, gates, square = arrive(2 * l, project)
        scale = lax.rsqrt(jnp.sum(square, axis=1, keepdims=True) / width + EPS)
        proj = proj * scale
        query = proj[:, :rows].astype(BF16)
        keyrow = (proj[:, rows : 2 * rows] * head ** (-0.5)).astype(BF16)
        pair[l, core, 0] = query
        pair[l, core, 1] = keyrow
        pair_send = pltpu.make_async_remote_copy(
            src_ref=pair.at[l, core],
            dst_ref=pair.at[l, core],
            send_sem=psend.at[l],
            recv_sem=precv.at[l],
            device_id={"tp": sibling},
            device_id_type=MESH,
        )
        pair_send.start()
        value = proj[:, 2 * rows : 3 * rows].astype(BF16).astype(F32)
        outgate = proj[:, 3 * rows : 4 * rows].astype(BF16).astype(F32)
        gates = gates * scale
        ingate = gates[:, :heads] + ingate_bias_in[l : l + 1, :]
        logit = (
            gates[:, heads : 2 * heads]
            + forget_bias_in[l : l + 1, :]
            + forget_slope_in[l : l + 1, :] * position
        )
        forget = jnp.minimum(logit, 0.0) - jnp.log1p(jnp.exp(-jnp.abs(logit)))
        shifted = forget + old_stab
        stab = jnp.maximum(shifted, ingate)
        decay = jnp.sum(
            jnp.where(head_mask, jnp.exp(shifted - stab), 0.0), axis=1, keepdims=True
        )
        inweight = jnp.sum(
            jnp.where(head_mask, jnp.exp(ingate - stab), 0.0), axis=1, keepdims=True
        )
        new_sums[l] = decay * sums[core, l] + inweight * keyrow.astype(F32)
        vt_ref[...] = jnp.concatenate((value, jnp.zeros((rows - batch, rows), F32)), axis=0).T
        decay_ref[...] = jnp.broadcast_to(decay, (batch, head))
        gate = (
            head_gain_in[...].astype(F32)[l : l + 1] * jax.nn.sigmoid(outgate)
        )

        pair_send.wait_send()
        sib_pair = pltpu.make_async_remote_copy(
            src_ref=pair.at[l, 1 - core],
            dst_ref=pair.at[l, 1 - core],
            send_sem=psend.at[l],
            recv_sem=precv.at[l],
            device_id={"tp": sibling},
            device_id_type=MESH,
        )
        sib_pair.wait_recv()
        if l == 0:
            sums_send.wait()
        head_query = jnp.concatenate((pair[l, 0, 0], pair[l, 1, 0]), axis=1)
        head_key = jnp.concatenate((pair[l, 0, 1], pair[l, 1, 1]), axis=1).astype(F32)
        query_float = head_query.astype(F32)
        kk_ref[...] = inweight * head_key
        key_dot = jnp.sum(head_key * query_float, axis=1, keepdims=True)
        old = jnp.concatenate((sums[0, l], sums[1, l]), axis=1)
        sum_dot = jnp.sum(old * query_float, axis=1, keepdims=True)
        denominator = jnp.maximum(jnp.abs(decay * sum_dot + inweight * key_dot), 1.0)
        padded = jnp.concatenate((head_query, jnp.zeros((rows - batch, head), BF16)), axis=0)

        mcopies[l].wait()
        lane = lax.broadcasted_iota(jnp.int32, (rows, rows), 1)

        def read(g, acc, l=l, padded=padded, lane=lane):
            at = g * GROUP
            c = mem[l, pl.ds(at, GROUP)].reshape(GROUP * rows, head).astype(BF16)
            r = lax.dot_general(
                c, padded, (((1,), (1,)), ((), ())), preferred_element_type=F32
            ).reshape(GROUP, rows, rows)
            for i in range(GROUP):
                acc = jnp.where(lane == at + i, r[i], acc)
            return acc

        readout = lax.fori_loop(0, batch // GROUP, read, jnp.zeros((rows, rows), F32)).T[:batch]
        hidden = (decay * readout + (inweight * key_dot) * value) / denominator
        gath[2 * l + 1, me] = (hidden * gate).astype(BF16)
        send_own(2 * l + 1)
        new_stab[l] = stab.T

        @pl.loop(0, batch // GROUP)
        def _(g, l=l):
            at = g * GROUP
            v = pltpu.roll(vt_ref[...], lax.rem(rows - at, rows), 1)
            for i in range(GROUP):
                mem[l, at + i] = mem[l, at + i] * decay_ref[pl.ds(at + i, 1), :] + v[
                    :, i : i + 1
                ] * kk_ref[pl.ds(at + i, 1), :]

        wcopies[l][6].wait()

        def output(c, total, l=l):
            at = pl.ds(lanes(c * 2 * rows, 2 * rows), 2 * rows)
            x = jnp.concatenate((gath[2 * l + 1, 2 * c], gath[2 * l + 1, 2 * c + 1]), axis=1)
            part = jnp.dot(x, wout[l, at, :], preferred_element_type=F32)
            return part if total is None else total + part

        moved = arrive(2 * l + 1, output)
        nxt = (current + moved).astype(BF16)
        current = nxt.astype(F32)
        if l + 1 < blocks:
            gath[2 * l + 2, me] = nxt
            send_own(2 * l + 2)
        else:
            new_tokens[...] = nxt

    for c in sent:
        c.wait_send()


def from_partner(value, axis, stride):
    mask = 2**stride
    pairs = [(source, source ^ mask) for source in range(lax.axis_size(axis))]
    return lax.ppermute(value, axis, pairs)


def plain_body(
    tokens,
    lengths,
    cell_memory,
    key_sums,
    stabilizer,
    norm_gain,
    query_weight,
    key_weight,
    value_weight,
    outgate_weight,
    ingate_weight,
    forget_weight,
    ingate_bias,
    forget_bias,
    forget_slope,
    head_gain,
    output_weight,
):
    devices = lax.axis_size("tp")
    split_count = devices // HEADS
    own_index = lax.axis_index("tp")
    head_id = own_index // split_count
    onehot = (jnp.arange(HEADS) == head_id).astype(jnp.float32)
    position = lengths.astype(jnp.float32) / MAXLEN
    current = tokens
    memories, sums_list, stabs = ([], [], [])
    for block_id in range(cell_memory.shape[0]):
        gathered_rows = lax.all_gather(current, "tp", axis=1, tiled=True)
        row_float = gathered_rows.astype(jnp.float32)
        normed = (
            row_float
            * lax.rsqrt(jnp.mean(row_float * row_float, axis=-1, keepdims=True) + EPS)
            * norm_gain[block_id].astype(jnp.float32)
        ).astype(jnp.bfloat16)
        queries = jnp.dot(
            normed, query_weight[block_id], preferred_element_type=jnp.float32
        ).astype(jnp.bfloat16)
        key_rows = (
            jnp.dot(normed, key_weight[block_id], preferred_element_type=jnp.float32)
            * HEAD ** (-0.5)
        ).astype(jnp.bfloat16)
        values = jnp.dot(normed, value_weight[block_id], preferred_element_type=jnp.float32).astype(
            jnp.bfloat16
        )
        outgate = jnp.dot(
            normed, outgate_weight[block_id], preferred_element_type=jnp.float32
        ).astype(jnp.bfloat16)
        ingate = (
            jnp.dot(normed, ingate_weight[block_id], preferred_element_type=jnp.float32)
            + ingate_bias[block_id]
        )
        forget = jax.nn.log_sigmoid(
            jnp.dot(normed, forget_weight[block_id], preferred_element_type=jnp.float32)
            + forget_bias[block_id]
            + forget_slope[block_id] * position[:, None]
        )
        stab_new = jnp.maximum(forget + stabilizer[block_id], ingate)
        decays = jnp.exp(forget + stabilizer[block_id] - stab_new)
        in_weight = jnp.exp(ingate - stab_new)
        decay_own = jnp.sum(decays * onehot, axis=1)
        inweight_own = jnp.sum(in_weight * onehot, axis=1)
        sums_new = decay_own[:, None] * key_sums[block_id] + inweight_own[
            :, None
        ] * key_rows.astype(jnp.float32)
        head_pair = jnp.stack((queries, key_rows))
        head_sums = sums_new
        for level in range(split_count.bit_length() - 1):
            partner = from_partner(head_pair, "tp", level)
            upper = own_index // (1 << level) % 2 == 1
            lower_half = jnp.where(upper, partner, head_pair)
            upper_half = jnp.where(upper, head_pair, partner)
            head_pair = jnp.concatenate((lower_half, upper_half), axis=2)
            sums_mate = from_partner(head_sums, "tp", level)
            sums_low = jnp.where(upper, sums_mate, head_sums)
            sums_high = jnp.where(upper, head_sums, sums_mate)
            head_sums = jnp.concatenate((sums_low, sums_high), axis=1)
        head_query = head_pair[0].astype(jnp.float32)
        head_keys = head_pair[1].astype(jnp.float32)
        mem_new = (
            decay_own[:, None, None] * cell_memory[block_id]
            + inweight_own[:, None, None]
            * values.astype(jnp.float32)[:, :, None]
            * head_keys[:, None, :]
        )
        numerator = jnp.einsum("bvk,bk->bv", mem_new, head_query, precision=lax.Precision.HIGHEST)
        denominator = jnp.maximum(jnp.abs(jnp.sum(head_sums * head_query, axis=1)), 1.0)
        hidden = numerator / denominator[:, None]
        gated_out = (
            hidden
            * head_gain[block_id].astype(jnp.float32)
            * jax.nn.sigmoid(outgate.astype(jnp.float32))
        ).astype(jnp.bfloat16)
        out_weight = output_weight[block_id]
        projected = jnp.dot(
            lax.all_gather(gated_out, "tp", axis=1, tiled=True),
            out_weight,
            preferred_element_type=jnp.float32,
        )
        current = (current.astype(jnp.float32) + projected).astype(jnp.bfloat16)
        memories.append(mem_new)
        sums_list.append(sums_new)
        stabs.append(stab_new)
    return (current, jnp.stack(memories), jnp.stack(sums_list), jnp.stack(stabs))


def write_out(*refs):
    sems = refs[8]
    copies = [pltpu.make_async_copy(refs[i], refs[4 + i], sems.at[i]) for i in range(4)]
    for c in copies:
        c.start()
    for c in copies:
        c.wait()


def body(*args):
    tokens, lengths, cell_memory, key_sums, stabilizer = args[:5]
    n = lax.axis_size("tp")
    blocks, batch, rows, head = cell_memory.shape
    heads = stabilizer.shape[2]
    width = args[6].shape[1]
    if n != 2 * heads or rows < batch or rows % 128 or batch % GROUP:
        return plain_body(*args)
    vm = pl.BlockSpec(memory_space=pltpu.VMEM)
    anyspace = pl.BlockSpec(memory_space=pl.ANY)
    dma = pltpu.SemaphoreType.DMA
    in_specs = [pl.BlockSpec(memory_space=pltpu.HBM)] * 17
    results = pl.pallas_call(
        functools.partial(kernel, n),
        out_shape=(
            pltpu.VMEM((batch, rows), BF16),
            pltpu.VMEM(cell_memory.shape, F32),
            pltpu.VMEM(key_sums.shape, F32),
            pltpu.VMEM((blocks, heads, batch), F32),
        ),
        in_specs=in_specs,
        out_specs=(vm, vm, vm, vm),
        scratch_shapes=[
            pltpu.VMEM((1, batch), jnp.int32),
            pltpu.VMEM((blocks, heads, batch), F32),
            pltpu.VMEM((blocks, width), BF16),
            pltpu.VMEM((blocks, heads), F32),
            pltpu.VMEM((blocks, heads), F32),
            pltpu.VMEM((blocks, heads), F32),
            pltpu.VMEM((blocks, rows), BF16),
            pltpu.VMEM((blocks, width, 4 * rows), BF16),
            pltpu.VMEM((blocks, width, rows), BF16),
            pltpu.VMEM((blocks, heads, width), BF16),
            pltpu.VMEM((blocks, heads, width), BF16),
            pltpu.VMEM((blocks, 2 * heads, width), BF16),
            dma((7,)),
            pltpu.VMEM((2 * blocks, n, batch, rows), BF16),
            pltpu.VMEM((blocks, 2, 2, batch, rows), BF16),
            pltpu.VMEM((2, blocks, batch, rows), F32),
            pltpu.VMEM((rows, rows), F32),
            pltpu.VMEM((batch, head), F32),
            pltpu.VMEM((batch, head), F32),
            dma((blocks, 8)),
            dma((blocks,)),
            dma((2 * blocks, n // 2)),
            dma((2 * blocks, n // 2)),
            dma((2 * blocks, n)),
            dma((blocks,)),
            dma((blocks,)),
            dma,
            dma,
        ],
        compiler_params=pltpu.CompilerParams(
            collective_id=0, has_side_effects=True, vmem_limit_bytes=45500000
        ),
    )(
        tokens,
        lengths.reshape(1, batch),
        cell_memory,
        key_sums,
        stabilizer.swapaxes(1, 2),
        *args[5:10],
        args[10].swapaxes(1, 2),
        args[11].swapaxes(1, 2),
        *args[12:],
    )
    final = pl.pallas_call(
        write_out,
        out_shape=tuple(jax.ShapeDtypeStruct(r.shape, r.dtype) for r in results),
        in_specs=[anyspace] * 4,
        out_specs=(anyspace,) * 4,
        scratch_shapes=[dma((4,))],
        compiler_params=pltpu.CompilerParams(vmem_limit_bytes=1024 * 1024),
    )(*results)
    return (*final[:3], final[3].swapaxes(1, 2))


def solution(mesh):
    in_specs = (
        P("grp", "tp"),
        P("grp"),
        P(None, "grp", "tp", None),
        P(None, "grp", "tp"),
        P(None, "grp", None),
        P(),
        P(None, None, "tp"),
        P(None, None, "tp"),
        P(None, None, "tp"),
        P(None, None, "tp"),
        P(),
        P(),
        P(),
        P(),
        P(),
        P(None, "tp"),
        P(None, None, "tp"),
    )
    out_specs = (
        P("grp", "tp"),
        P(None, "grp", "tp", None),
        P(None, "grp", "tp"),
        P(None, "grp", None),
    )
    return jax.shard_map(body, mesh=mesh, in_specs=in_specs, out_specs=out_specs, check_vma=False)
```

```python
import functools

import jax
import jax.numpy as jnp
from jax import lax
from jax.experimental import pallas as pl
from jax.experimental.pallas import tpu as pltpu
from jax.sharding import PartitionSpec as P

HEADS = 8
HEAD = 256
MAXLEN = 4096
EPS = 1e-05
MESH = pl.DeviceIdType.MESH
F32 = jnp.float32
BF16 = jnp.bfloat16
GROUP = 8


def kernel(
    n,
    tokens,
    lengths,
    cell_memory,
    key_sums,
    stabilizer,
    norm_gain,
    query_weight,
    key_weight,
    value_weight,
    outgate_weight,
    ingate_weight,
    forget_weight,
    ingate_bias,
    forget_bias,
    forget_slope,
    head_gain,
    output_weight,
    new_tokens,
    mem,
    new_sums,
    new_stab,
    lengths_in,
    stabilizer_in,
    norm_gain_in,
    ingate_bias_in,
    forget_bias_in,
    forget_slope_in,
    head_gain_in,
    wbig,
    wout,
    wgi,
    wgf,
    wgate,
    small_sem,
    gath,
    pair,
    sums,
    vt_ref,
    decay_ref,
    kk_ref,
    local_sem,
    mem_sem,
    gsend,
    gfwd,
    grecv,
    psend,
    precv,
    ssend,
    srecv,
):
    blocks, batch, rows, head = mem.shape
    heads = stabilizer.shape[1]
    width = output_weight.shape[1]
    split = n // heads
    chips = n // 2
    me = lax.axis_index("tp")
    chip = me // 2
    core = lax.rem(me, 2)
    sibling = me + 1 - 2 * core
    own_head = me // split
    lanes = pl.multiple_of

    def target(j):
        return lax.rem(chip + j, chips) * 2 + core

    def source(j):
        return lax.rem(chip + chips - j, chips) * 2 + core

    own_copy = pltpu.make_async_copy(tokens, gath.at[0, me], local_sem.at[0, 7])
    own_copy.start()
    sums_copy = pltpu.make_async_copy(key_sums, sums.at[core], local_sem.at[1, 7])
    sums_copy.start()
    small = [
        pltpu.make_async_copy(a, b, small_sem.at[i])
        for i, (a, b) in enumerate(
            (
                (lengths, lengths_in),
                (stabilizer, stabilizer_in),
                (norm_gain, norm_gain_in),
                (ingate_bias, ingate_bias_in),
                (forget_bias, forget_bias_in),
                (forget_slope, forget_slope_in),
                (head_gain, head_gain_in),
            )
        )
    ]
    for c in small:
        c.start()
    wcopies, mcopies = [], []
    for l in range(blocks):
        now = []
        for i, w in enumerate((query_weight, key_weight, value_weight, outgate_weight)):
            now.append(
                pltpu.make_async_copy(
                    w.at[l], wbig.at[l, :, pl.ds(i * rows, rows)], local_sem.at[l, i]
                )
            )
        now.append(pltpu.make_async_copy(ingate_weight.at[l], wgi.at[l], local_sem.at[l, 4]))
        now.append(pltpu.make_async_copy(forget_weight.at[l], wgf.at[l], local_sem.at[l, 5]))
        now.append(pltpu.make_async_copy(output_weight.at[l], wout.at[l], local_sem.at[l, 6]))
        wcopies.append(now)
        mcopies.append(pltpu.make_async_copy(cell_memory.at[l], mem.at[l], mem_sem.at[l]))
        for c in now:
            c.start()
        mcopies[l].start()

    barrier = pltpu.get_barrier_semaphore()
    pl.semaphore_signal(barrier, inc=1, device_id={"tp": sibling}, device_id_type=MESH)
    for j in range(1, chips):
        pl.semaphore_signal(barrier, inc=1, device_id={"tp": target(j)}, device_id_type=MESH)
    pl.semaphore_wait(barrier, chips)

    def block_copy(g, slot, sems, k, dest):
        return pltpu.make_async_remote_copy(
            src_ref=gath.at[g, slot],
            dst_ref=gath.at[g, slot],
            send_sem=sems.at[g, k],
            recv_sem=grecv.at[g, slot],
            device_id={"tp": dest},
            device_id_type=MESH,
        )

    sent = []

    def send_own(g):
        for j in range(1, chips):
            c = block_copy(g, me, gsend, j, target(j))
            c.start()
            sent.append(c)
        c = block_copy(g, me, gsend, 0, sibling)
        c.start()
        sent.append(c)

    def arrive(g, step):
        total = None
        block_copy(g, sibling, gsend, 0, sibling).wait_recv()
        total = step(chip, total)
        for j in range(1, chips):
            s = source(j)
            block_copy(g, s, gsend, j, sibling).wait_recv()
            c = block_copy(g, s, gfwd, j, sibling)
            c.start()
            sent.append(c)
        for j in range(1, chips):
            s = source(j)
            block_copy(g, s + 1 - 2 * core, gsend, j, sibling).wait_recv()
            total = step(s // 2, total)
        return total

    own_copy.wait()
    send_own(0)
    sums_copy.wait()
    sums_send = pltpu.make_async_remote_copy(
        src_ref=sums.at[core],
        dst_ref=sums.at[core],
        send_sem=ssend,
        recv_sem=srecv,
        device_id={"tp": sibling},
        device_id_type=MESH,
    )
    sums_send.start()

    for c in small:
        c.wait()
    eye = lax.broadcasted_iota(jnp.int32, (batch, batch), 0) == lax.broadcasted_iota(
        jnp.int32, (batch, batch), 1
    )
    position = jnp.sum(
        jnp.where(eye, lengths_in[...].astype(F32) / MAXLEN, 0.0), axis=1, keepdims=True
    )
    head_mask = lax.broadcasted_iota(jnp.int32, (batch, heads), 1) == own_head
    current = gath[0, me].astype(F32)

    for l in range(blocks):
        for c in wcopies[l][:6]:
            c.wait()
        wgate[l] = jnp.concatenate((wgi[l].astype(F32), wgf[l].astype(F32)), axis=0).astype(BF16)
        old_stab = stabilizer_in[l].T

        def project(c, total, l=l):
            at = pl.ds(lanes(c * 2 * rows, 2 * rows), 2 * rows)
            x = jnp.concatenate((gath[2 * l, 2 * c], gath[2 * l, 2 * c + 1]), axis=1).astype(F32)
            gain = norm_gain_in[:, at].astype(F32)[l : l + 1]
            scaled = (x * gain).astype(BF16)
            part = jnp.dot(scaled, wbig[l, at, :], preferred_element_type=F32)
            gpart = lax.dot_general(
                scaled, wgate[l, :, at], (((1,), (1,)), ((), ())), preferred_element_type=F32
            )
            square = x * x
            if total is None:
                return part, gpart, square
            return total[0] + part, total[1] + gpart, total[2] + square

        proj, gates, square = arrive(2 * l, project)
        scale = lax.rsqrt(jnp.sum(square, axis=1, keepdims=True) / width + EPS)
        proj = proj * scale
        query = proj[:, :rows].astype(BF16)
        keyrow = (proj[:, rows : 2 * rows] * head ** (-0.5)).astype(BF16)
        pair[l, core, 0] = query
        pair[l, core, 1] = keyrow
        pair_send = pltpu.make_async_remote_copy(
            src_ref=pair.at[l, core],
            dst_ref=pair.at[l, core],
            send_sem=psend.at[l],
            recv_sem=precv.at[l],
            device_id={"tp": sibling},
            device_id_type=MESH,
        )
        pair_send.start()
        value = proj[:, 2 * rows : 3 * rows].astype(BF16).astype(F32)
        outgate = proj[:, 3 * rows : 4 * rows].astype(BF16).astype(F32)
        gates = gates * scale
        ingate = gates[:, :heads] + ingate_bias_in[l : l + 1, :]
        logit = (
            gates[:, heads : 2 * heads]
            + forget_bias_in[l : l + 1, :]
            + forget_slope_in[l : l + 1, :] * position
        )
        forget = jnp.minimum(logit, 0.0) - jnp.log1p(jnp.exp(-jnp.abs(logit)))
        shifted = forget + old_stab
        stab = jnp.maximum(shifted, ingate)
        decay = jnp.sum(
            jnp.where(head_mask, jnp.exp(shifted - stab), 0.0), axis=1, keepdims=True
        )
        inweight = jnp.sum(
            jnp.where(head_mask, jnp.exp(ingate - stab), 0.0), axis=1, keepdims=True
        )
        new_sums[l] = decay * sums[core, l] + inweight * keyrow.astype(F32)
        vt_ref[...] = jnp.concatenate((value, jnp.zeros((rows - batch, rows), F32)), axis=0).T
        decay_ref[...] = jnp.broadcast_to(decay, (batch, head))
        gate = (
            head_gain_in[...].astype(F32)[l : l + 1] * jax.nn.sigmoid(outgate)
        )

        pair_send.wait_send()
        sib_pair = pltpu.make_async_remote_copy(
            src_ref=pair.at[l, 1 - core],
            dst_ref=pair.at[l, 1 - core],
            send_sem=psend.at[l],
            recv_sem=precv.at[l],
            device_id={"tp": sibling},
            device_id_type=MESH,
        )
        sib_pair.wait_recv()
        if l == 0:
            sums_send.wait()
        head_query = jnp.concatenate((pair[l, 0, 0], pair[l, 1, 0]), axis=1)
        head_key = jnp.concatenate((pair[l, 0, 1], pair[l, 1, 1]), axis=1).astype(F32)
        query_float = head_query.astype(F32)
        kk_ref[...] = inweight * head_key
        key_dot = jnp.sum(head_key * query_float, axis=1, keepdims=True)
        old = jnp.concatenate((sums[0, l], sums[1, l]), axis=1)
        sum_dot = jnp.sum(old * query_float, axis=1, keepdims=True)
        denominator = jnp.maximum(jnp.abs(decay * sum_dot + inweight * key_dot), 1.0)
        padded = jnp.concatenate((head_query, jnp.zeros((rows - batch, head), BF16)), axis=0)

        mcopies[l].wait()
        lane = lax.broadcasted_iota(jnp.int32, (rows, rows), 1)

        def read(g, acc, l=l, padded=padded, lane=lane):
            at = g * GROUP
            c = mem[l, pl.ds(at, GROUP)].reshape(GROUP * rows, head).astype(BF16)
            r = lax.dot_general(
                c, padded, (((1,), (1,)), ((), ())), preferred_element_type=F32
            ).reshape(GROUP, rows, rows)
            for i in range(GROUP):
                acc = jnp.where(lane == at + i, r[i], acc)
            return acc

        readout = lax.fori_loop(0, batch // GROUP, read, jnp.zeros((rows, rows), F32), unroll=5).T[:batch]
        hidden = (decay * readout + (inweight * key_dot) * value) / denominator
        gath[2 * l + 1, me] = (hidden * gate).astype(BF16)
        send_own(2 * l + 1)
        new_stab[l] = stab.T

        @pl.loop(0, batch // GROUP)
        def _(g, l=l):
            at = g * GROUP
            v = pltpu.roll(vt_ref[...], lax.rem(rows - at, rows), 1)
            for i in range(GROUP):
                mem[l, at + i] = mem[l, at + i] * decay_ref[pl.ds(at + i, 1), :] + v[
                    :, i : i + 1
                ] * kk_ref[pl.ds(at + i, 1), :]

        wcopies[l][6].wait()

        def output(c, total, l=l):
            at = pl.ds(lanes(c * 2 * rows, 2 * rows), 2 * rows)
            x = jnp.concatenate((gath[2 * l + 1, 2 * c], gath[2 * l + 1, 2 * c + 1]), axis=1)
            part = jnp.dot(x, wout[l, at, :], preferred_element_type=F32)
            return part if total is None else total + part

        moved = arrive(2 * l + 1, output)
        nxt = (current + moved).astype(BF16)
        current = nxt.astype(F32)
        if l + 1 < blocks:
            gath[2 * l + 2, me] = nxt
            send_own(2 * l + 2)
        else:
            new_tokens[...] = nxt

    for c in sent:
        c.wait_send()


def from_partner(value, axis, stride):
    mask = 2**stride
    pairs = [(source, source ^ mask) for source in range(lax.axis_size(axis))]
    return lax.ppermute(value, axis, pairs)


def plain_body(
    tokens,
    lengths,
    cell_memory,
    key_sums,
    stabilizer,
    norm_gain,
    query_weight,
    key_weight,
    value_weight,
    outgate_weight,
    ingate_weight,
    forget_weight,
    ingate_bias,
    forget_bias,
    forget_slope,
    head_gain,
    output_weight,
):
    devices = lax.axis_size("tp")
    split_count = devices // HEADS
    own_index = lax.axis_index("tp")
    head_id = own_index // split_count
    onehot = (jnp.arange(HEADS) == head_id).astype(jnp.float32)
    position = lengths.astype(jnp.float32) / MAXLEN
    current = tokens
    memories, sums_list, stabs = ([], [], [])
    for block_id in range(cell_memory.shape[0]):
        gathered_rows = lax.all_gather(current, "tp", axis=1, tiled=True)
        row_float = gathered_rows.astype(jnp.float32)
        normed = (
            row_float
            * lax.rsqrt(jnp.mean(row_float * row_float, axis=-1, keepdims=True) + EPS)
            * norm_gain[block_id].astype(jnp.float32)
        ).astype(jnp.bfloat16)
        queries = jnp.dot(
            normed, query_weight[block_id], preferred_element_type=jnp.float32
        ).astype(jnp.bfloat16)
        key_rows = (
            jnp.dot(normed, key_weight[block_id], preferred_element_type=jnp.float32)
            * HEAD ** (-0.5)
        ).astype(jnp.bfloat16)
        values = jnp.dot(normed, value_weight[block_id], preferred_element_type=jnp.float32).astype(
            jnp.bfloat16
        )
        outgate = jnp.dot(
            normed, outgate_weight[block_id], preferred_element_type=jnp.float32
        ).astype(jnp.bfloat16)
        ingate = (
            jnp.dot(normed, ingate_weight[block_id], preferred_element_type=jnp.float32)
            + ingate_bias[block_id]
        )
        forget = jax.nn.log_sigmoid(
            jnp.dot(normed, forget_weight[block_id], preferred_element_type=jnp.float32)
            + forget_bias[block_id]
            + forget_slope[block_id] * position[:, None]
        )
        stab_new = jnp.maximum(forget + stabilizer[block_id], ingate)
        decays = jnp.exp(forget + stabilizer[block_id] - stab_new)
        in_weight = jnp.exp(ingate - stab_new)
        decay_own = jnp.sum(decays * onehot, axis=1)
        inweight_own = jnp.sum(in_weight * onehot, axis=1)
        sums_new = decay_own[:, None] * key_sums[block_id] + inweight_own[
            :, None
        ] * key_rows.astype(jnp.float32)
        head_pair = jnp.stack((queries, key_rows))
        head_sums = sums_new
        for level in range(split_count.bit_length() - 1):
            partner = from_partner(head_pair, "tp", level)
            upper = own_index // (1 << level) % 2 == 1
            lower_half = jnp.where(upper, partner, head_pair)
            upper_half = jnp.where(upper, head_pair, partner)
            head_pair = jnp.concatenate((lower_half, upper_half), axis=2)
            sums_mate = from_partner(head_sums, "tp", level)
            sums_low = jnp.where(upper, sums_mate, head_sums)
            sums_high = jnp.where(upper, head_sums, sums_mate)
            head_sums = jnp.concatenate((sums_low, sums_high), axis=1)
        head_query = head_pair[0].astype(jnp.float32)
        head_keys = head_pair[1].astype(jnp.float32)
        mem_new = (
            decay_own[:, None, None] * cell_memory[block_id]
            + inweight_own[:, None, None]
            * values.astype(jnp.float32)[:, :, None]
            * head_keys[:, None, :]
        )
        numerator = jnp.einsum("bvk,bk->bv", mem_new, head_query, precision=lax.Precision.HIGHEST)
        denominator = jnp.maximum(jnp.abs(jnp.sum(head_sums * head_query, axis=1)), 1.0)
        hidden = numerator / denominator[:, None]
        gated_out = (
            hidden
            * head_gain[block_id].astype(jnp.float32)
            * jax.nn.sigmoid(outgate.astype(jnp.float32))
        ).astype(jnp.bfloat16)
        out_weight = output_weight[block_id]
        projected = jnp.dot(
            lax.all_gather(gated_out, "tp", axis=1, tiled=True),
            out_weight,
            preferred_element_type=jnp.float32,
        )
        current = (current.astype(jnp.float32) + projected).astype(jnp.bfloat16)
        memories.append(mem_new)
        sums_list.append(sums_new)
        stabs.append(stab_new)
    return (current, jnp.stack(memories), jnp.stack(sums_list), jnp.stack(stabs))


def write_out(*refs):
    sems = refs[8]
    copies = [pltpu.make_async_copy(refs[i], refs[4 + i], sems.at[i]) for i in (0, 2, 3)]
    blocks, batch = refs[1].shape[:2]
    for l in range(blocks):
        for g in range(batch // GROUP):
            at = pl.ds(g * GROUP, GROUP)
            copies.append(
                pltpu.make_async_copy(
                    refs[1].at[l, at], refs[5].at[l, at], sems.at[4 + l * (batch // GROUP) + g]
                )
            )
    for c in copies:
        c.start()
    for c in copies:
        c.wait()


def body(*args):
    tokens, lengths, cell_memory, key_sums, stabilizer = args[:5]
    n = lax.axis_size("tp")
    blocks, batch, rows, head = cell_memory.shape
    heads = stabilizer.shape[2]
    width = args[6].shape[1]
    if n != 2 * heads or rows < batch or rows % 128 or batch % GROUP:
        return plain_body(*args)
    vm = pl.BlockSpec(memory_space=pltpu.VMEM)
    anyspace = pl.BlockSpec(memory_space=pl.ANY)
    dma = pltpu.SemaphoreType.DMA
    in_specs = [pl.BlockSpec(memory_space=pltpu.HBM)] * 17
    results = pl.pallas_call(
        functools.partial(kernel, n),
        out_shape=(
            pltpu.VMEM((batch, rows), BF16),
            pltpu.VMEM(cell_memory.shape, F32),
            pltpu.VMEM(key_sums.shape, F32),
            pltpu.VMEM((blocks, heads, batch), F32),
        ),
        in_specs=in_specs,
        out_specs=(vm, vm, vm, vm),
        scratch_shapes=[
            pltpu.VMEM((1, batch), jnp.int32),
            pltpu.VMEM((blocks, heads, batch), F32),
            pltpu.VMEM((blocks, width), BF16),
            pltpu.VMEM((blocks, heads), F32),
            pltpu.VMEM((blocks, heads), F32),
            pltpu.VMEM((blocks, heads), F32),
            pltpu.VMEM((blocks, rows), BF16),
            pltpu.VMEM((blocks, width, 4 * rows), BF16),
            pltpu.VMEM((blocks, width, rows), BF16),
            pltpu.VMEM((blocks, heads, width), BF16),
            pltpu.VMEM((blocks, heads, width), BF16),
            pltpu.VMEM((blocks, 2 * heads, width), BF16),
            dma((7,)),
            pltpu.VMEM((2 * blocks, n, batch, rows), BF16),
            pltpu.VMEM((blocks, 2, 2, batch, rows), BF16),
            pltpu.VMEM((2, blocks, batch, rows), F32),
            pltpu.VMEM((rows, rows), F32),
            pltpu.VMEM((batch, head), F32),
            pltpu.VMEM((batch, head), F32),
            dma((blocks, 8)),
            dma((blocks,)),
            dma((2 * blocks, n // 2)),
            dma((2 * blocks, n // 2)),
            dma((2 * blocks, n)),
            dma((blocks,)),
            dma((blocks,)),
            dma,
            dma,
        ],
        compiler_params=pltpu.CompilerParams(
            collective_id=0, has_side_effects=True, vmem_limit_bytes=45500000
        ),
    )(
        tokens,
        lengths.reshape(1, batch),
        cell_memory,
        key_sums,
        stabilizer.swapaxes(1, 2),
        *args[5:10],
        args[10].swapaxes(1, 2),
        args[11].swapaxes(1, 2),
        *args[12:],
    )
    final = pl.pallas_call(
        write_out,
        out_shape=tuple(jax.ShapeDtypeStruct(r.shape, r.dtype) for r in results),
        in_specs=[anyspace] * 4,
        out_specs=(anyspace,) * 4,
        scratch_shapes=[dma((4 + blocks * (batch // GROUP),))],
        compiler_params=pltpu.CompilerParams(vmem_limit_bytes=1024 * 1024),
    )(*results)
    return (*final[:3], final[3].swapaxes(1, 2))


def solution(mesh):
    in_specs = (
        P("grp", "tp"),
        P("grp"),
        P(None, "grp", "tp", None),
        P(None, "grp", "tp"),
        P(None, "grp", None),
        P(),
        P(None, None, "tp"),
        P(None, None, "tp"),
        P(None, None, "tp"),
        P(None, None, "tp"),
        P(),
        P(),
        P(),
        P(),
        P(),
        P(None, "tp"),
        P(None, None, "tp"),
    )
    out_specs = (
        P("grp", "tp"),
        P(None, "grp", "tp", None),
        P(None, "grp", "tp"),
        P(None, "grp", None),
    )
    return jax.shard_map(body, mesh=mesh, in_specs=in_specs, out_specs=out_specs, check_vma=False)
```
